32 devices in a mesh: sp: 4 (over z), fs: 4 (over y, x), tp: 2 (over core).
Axes of the slice: x: 2, y: 2, z: 4, core: 2. Of those that a mesh axis runs over, the one named last changes fastest.
Arguments:
- tokens: bfloat16 [4, 3072, 2048], P('fs', 'sp'), may hold values from -6 to 6
- norm_gain: float32 [2048], replicated, may hold values from 0.1 to 1.9
- query_weight: bfloat16 [2048, 512], P(('sp', 'fs'), 'tp'), may hold values from -0.125 to 0.125
- key_weight: bfloat16 [2048, 512], P(('sp', 'fs'), 'tp'), may hold values from -0.125 to 0.125
- value_weight: bfloat16 [2048, 1024], P(('sp', 'fs'), 'tp'), may hold values from -0.125 to 0.125
- gate_weight: bfloat16 [2048, 1024], P(('sp', 'fs'), 'tp'), may hold values from -0.125 to 0.125
- conv_b_weight: bfloat16 [2048, 1024], P(('sp', 'fs'), 'tp'), may hold values from -0.125 to 0.125
- conv_c_weight: bfloat16 [2048, 1024], P(('sp', 'fs'), 'tp'), may hold values from -0.125 to 0.125
- conv_in_weight: bfloat16 [2048, 1024], P(('sp', 'fs'), 'tp'), may hold values from -0.125 to 0.125
- conv_kernel: float32 [3, 1024], P(None, 'tp'), may hold values from -3.5 to 3.5
- out_ret_weight: bfloat16 [2048, 1024], P(('sp', 'fs'), 'tp'), may hold values from -0.125 to 0.125
- out_conv_weight: bfloat16 [2048, 1024], P(('sp', 'fs'), 'tp'), may hold values from -0.125 to 0.125
- log_decay: float32 [4, 8, 3072], P('fs', 'tp', 'sp'), may hold values from -3 to 0, as said below
Outputs:
- mixed: bfloat16 [4, 3072, 2048], P('fs', ('sp', 'tp'))
The draws below stay inside these ranges and needn't reach their ends.
Inputs may be any that keep to these rules, and one draw needn't show every extreme that they name: log_decay is never positive.
All inputs are finite; a program needn't handle non-finite values.
Results may differ from the reference program's by a relative error of at most 0.02.
Values may be sent and summed in bfloat16 or wider, within the bound.
No kernel may reach another device: no remote copies, remote signals or barrier semaphores. Data moves between devices by JAX's collectives and lax.ppermute only.
A program may use at most 64 MiB of HBM per device.

```python
import jax
import jax.numpy as jnp
from jax import lax

MODEL = 2048
MEMORY_CHANNELS = 8
KEY_DIM = 64
VALUE_DIM = 128
CONV_DIM = 1024
CONV_TAPS = 3
BLOCK_LEN = 128
TOK_DEV = 768
SERIES_NUMBER = 4
SERIES_SPAN = 3072
N_TP = 2


def draw_log_decay(key, part):
    lookup_matrix_lines = jax.random.split(jax.random.fold_in(key, 17), 7)
    head_shape = (SERIES_NUMBER, MEMORY_CHANNELS, 1)
    fast_share = 0.5
    is_fast = jax.random.uniform(lookup_matrix_lines[0], head_shape, jnp.float32) < fast_share
    fast_rate = jnp.exp(jax.random.uniform(lookup_matrix_lines[1], head_shape, jnp.float32, jnp.log(0.04), jnp.log(0.1)))
    slow_rate = jnp.exp(jax.random.uniform(lookup_matrix_lines[2], head_shape, jnp.float32, jnp.log(0.1), jnp.log(0.25))) / SERIES_SPAN
    background_frequency = jnp.where(is_fast, fast_rate, slow_rate)
    segment_multiplier = jnp.exp(jax.random.uniform(lookup_matrix_lines[3], (SERIES_NUMBER, MEMORY_CHANNELS, SERIES_SPAN // TOK_DEV), jnp.float32, -0.7, 0.7))
    segment_multiplier = jnp.repeat(segment_multiplier, TOK_DEV, axis=-1)
    noise_magnitude = jax.random.uniform(lookup_matrix_lines[4], (SERIES_NUMBER, MEMORY_CHANNELS, SERIES_SPAN), jnp.float32, 0.4, 1.6)
    spike_places = jax.random.randint(lookup_matrix_lines[5], (SERIES_NUMBER, MEMORY_CHANNELS, 3), 0, SERIES_SPAN)
    spike_magnitude = jnp.log(jax.random.uniform(lookup_matrix_lines[6], (SERIES_NUMBER, MEMORY_CHANNELS, 3), jnp.float32, 0.55, 0.8))
    token_ordinal = jnp.arange(SERIES_SPAN)
    spike_occurrences = jnp.sum(jnp.where(token_ordinal[None, None, :, None] == spike_places[:, :, None, :], spike_magnitude[:, :, None, :], 0.0), axis=-1)
    return (spike_occurrences - background_frequency * segment_multiplier * noise_magnitude).astype(jnp.float32)


def block_levels(rng, extent, pieces, smallest, top_value):
    gain, own = 1.0, jax.random.fold_in(rng, 6)
    for axis_at, shards_of in pieces:
        draws = jnp.exp(jax.random.uniform(jax.random.fold_in(own, axis_at), (shards_of,), jnp.float32, smallest / len(pieces), top_value / len(pieces)))
        gain = gain * jnp.repeat(draws, extent[axis_at] // shards_of).reshape([-1 if axis == axis_at else 1 for axis in range(len(extent))])
    return gain


def noise(stream_key, dims, width, bound, cuts=(), kind=jnp.bfloat16):
    values = jax.random.normal(stream_key, dims, jnp.float32) * width
    if len(cuts) > 0:
        values = block_levels(stream_key, dims, cuts, -0.22, 0.18) * values
    return jnp.clip(values, min=-bound, max=bound).astype(kind)


def setup_inputs(seed: int = 0) -> dict:
    keys = jax.random.split(jax.random.key(seed), 14)
    return {
        "tokens": noise(keys[0], (SERIES_NUMBER, SERIES_SPAN, MODEL), 1.0, 6.0, ((0, 4), (1, 4))),
        "norm_gain": jnp.clip(1.0 + 0.18 * jax.random.normal(keys[1], (MODEL,), jnp.float32), 0.1, 1.9),
        "query_weight": noise(keys[2], (MODEL, MEMORY_CHANNELS * KEY_DIM), MODEL ** -0.5, 0.125, ((0, 16), (1, 2))),
        "key_weight": noise(keys[3], (MODEL, MEMORY_CHANNELS * KEY_DIM), MODEL ** -0.5, 0.125, ((0, 16), (1, 2))),
        "value_weight": noise(keys[4], (MODEL, MEMORY_CHANNELS * VALUE_DIM), MODEL ** -0.5, 0.125, ((0, 16), (1, 2))),
        "gate_weight": noise(keys[5], (MODEL, MEMORY_CHANNELS * VALUE_DIM), MODEL ** -0.5, 0.125, ((0, 16), (1, 2))),
        "conv_b_weight": noise(keys[6], (MODEL, CONV_DIM), MODEL ** -0.5, 0.125, ((0, 16), (1, 2))),
        "conv_c_weight": noise(keys[7], (MODEL, CONV_DIM), MODEL ** -0.5, 0.125, ((0, 16), (1, 2))),
        "conv_in_weight": noise(keys[8], (MODEL, CONV_DIM), MODEL ** -0.5, 0.125, ((0, 16), (1, 2))),
        "conv_kernel": noise(keys[9], (CONV_TAPS, CONV_DIM), CONV_TAPS ** -0.5, 3.5, ((1, 2),), jnp.float32),
        "out_ret_weight": noise(keys[10], (MODEL, MEMORY_CHANNELS * VALUE_DIM), (MEMORY_CHANNELS * VALUE_DIM + CONV_DIM) ** -0.5, 0.125, ((0, 16), (1, 2))),
        "out_conv_weight": noise(keys[11], (MODEL, CONV_DIM), (MEMORY_CHANNELS * VALUE_DIM + CONV_DIM) ** -0.5, 0.125, ((0, 16), (1, 2))),
        "log_decay": draw_log_decay(jax.random.fold_in(keys[13], 71), 0),
    }


EPSILON = 1e-06
ROPE_BASE = 10000.0

def to_half(values):
    return lax.optimization_barrier(values.astype(jnp.bfloat16))

def rotate(values, token_ordinal):
    half_dim = values.shape[-1] // 2
    frequency = 1.0 / ROPE_BASE ** jnp.linspace(0.0, 1.0, half_dim, dtype=jnp.float32)
    angles = token_ordinal[:, None] * frequency[None, :]
    cosine_table = jnp.cos(angles)[:, None, :]
    sine_table = jnp.sin(angles)[:, None, :]
    first = values[..., :half_dim].astype(jnp.float32)
    second = values[..., half_dim:].astype(jnp.float32)
    return jnp.concatenate([first * cosine_table - second * sine_table, first * sine_table + second * cosine_table], axis=-1)

def retention_pass(queries, lookup_matrix_lines, values, decays):
    length, head_count, key_dim = queries.shape
    blocks = length // BLOCK_LEN

    def split_blocks(array):
        shaped = array.reshape(blocks, BLOCK_LEN, head_count, array.shape[-1])
        return jnp.transpose(shaped, (0, 2, 1, 3)).astype(jnp.float32)
    query_blocks = split_blocks(queries)
    key_blocks = split_blocks(lookup_matrix_lines)
    value_blocks = split_blocks(values)
    decay_blocks = jnp.transpose(decays.reshape(head_count, blocks, BLOCK_LEN), (1, 0, 2))
    cumulative = jnp.cumsum(decay_blocks, axis=-1)
    ending = cumulative[..., -1:]
    decay_gaps = cumulative[..., :, None] - cumulative[..., None, :]
    causal = jnp.arange(BLOCK_LEN)[:, None] >= jnp.arange(BLOCK_LEN)[None, :]
    weighting = jnp.where(causal, jnp.exp(jnp.minimum(decay_gaps, 0.0)), 0.0)
    scores = to_half(jnp.einsum('nhid,nhjd->nhij', query_blocks, key_blocks) * weighting).astype(jnp.float32)
    intra_out = jnp.einsum('nhij,nhje->nhie', scores, value_blocks)
    decayed_keys = to_half(key_blocks * jnp.exp(ending - cumulative)[..., None]).astype(jnp.float32)
    decayed_queries = to_half(query_blocks * jnp.exp(cumulative)[..., None]).astype(jnp.float32)
    block_kv = jnp.einsum('nhjd,nhje->nhde', decayed_keys, value_blocks)

    def advance(state_now, step_in):
        kv_block, total = step_in
        return (state_now * jnp.exp(total)[:, None, None] + kv_block, state_now)
    start_state = jnp.zeros((head_count, key_dim, values.shape[-1]), jnp.float32)
    _, before = lax.scan(advance, start_state, (block_kv, ending[..., 0]))
    cross = jnp.einsum('nhid,nhde->nhie', decayed_queries, to_half(before).astype(jnp.float32))
    output = intra_out + cross
    output = output * lax.rsqrt(lax.optimization_barrier(jnp.mean(output * output, axis=-1, keepdims=True)) + EPSILON)
    return jnp.transpose(output, (0, 2, 1, 3)).reshape(length, head_count * output.shape[-1])

def reference(tokens, norm_gain, query_weight, key_weight, value_weight, gate_weight, conv_b_weight, conv_c_weight, conv_in_weight, conv_kernel, out_ret_weight, out_conv_weight, log_decay):

    def one_sequence(pair):
        sequence_tokens, sequence_decay = pair
        inputs = sequence_tokens.astype(jnp.float32)
        length = inputs.shape[0]
        normed = to_half(inputs * lax.rsqrt(lax.optimization_barrier(jnp.mean(inputs * inputs, axis=-1, keepdims=True)) + EPSILON) * norm_gain.astype(jnp.float32))

        def project(weight):
            return to_half(jnp.dot(normed, weight, preferred_element_type=jnp.float32))
        token_ordinal = jnp.arange(length, dtype=jnp.float32)
        query_raw = project(query_weight).reshape(length, MEMORY_CHANNELS, KEY_DIM)
        key_raw = project(key_weight).reshape(length, MEMORY_CHANNELS, KEY_DIM)
        value_proj = project(value_weight).reshape(length, MEMORY_CHANNELS, VALUE_DIM)
        queries = to_half(rotate(query_raw, token_ordinal))
        lookup_matrix_lines = to_half(rotate(key_raw, token_ordinal) * KEY_DIM ** (-0.5))
        retained = retention_pass(queries, lookup_matrix_lines, value_proj, sequence_decay)
        ret_out = to_half(retained * jax.nn.silu(project(gate_weight).astype(jnp.float32)))
        gate_b = project(conv_b_weight).astype(jnp.float32)
        gate_c = project(conv_c_weight).astype(jnp.float32)
        conv_input = project(conv_in_weight).astype(jnp.float32)
        product = gate_c * conv_input
        padded = jnp.concatenate([jnp.zeros((CONV_TAPS - 1, CONV_DIM), jnp.float32), product], axis=0)
        convolved = jnp.zeros((length, CONV_DIM), jnp.float32)
        for tap_index in range(CONV_TAPS):
            convolved = convolved + conv_kernel[tap_index].astype(jnp.float32) * padded[tap_index:tap_index + length]
        conv_out = to_half(gate_b * convolved)
        ret_group = MEMORY_CHANNELS * VALUE_DIM // N_TP
        conv_group = CONV_DIM // N_TP
        total = jnp.zeros((length, MODEL), jnp.float32)
        for group in range(N_TP):
            ret_cols = slice(group * ret_group, (group + 1) * ret_group)
            conv_cols = slice(group * conv_group, (group + 1) * conv_group)
            partial_value = jnp.dot(ret_out[:, ret_cols], out_ret_weight[:, ret_cols].T, preferred_element_type=jnp.float32)
            partial_value = partial_value + jnp.dot(conv_out[:, conv_cols], out_conv_weight[:, conv_cols].T, preferred_element_type=jnp.float32)
            total = total + to_half(partial_value).astype(jnp.float32)
        return total.astype(jnp.bfloat16)
    return lax.map(one_sequence, (tokens, log_decay))
```

```python
import functools

import jax
import jax.numpy as jnp
from jax import lax
from jax.experimental import pallas as pl
from jax.experimental.pallas import tpu as pltpu
from jax.sharding import PartitionSpec as P

KEY_DIM = 64
VALUE_DIM = 128
CONV_TAPS = 3
BLOCK_LEN = 128
LANES = 128

EPSILON = 1e-06
ROPE_BASE = 10000.0


def vmem(mib):
    return pltpu.CompilerParams(vmem_limit_bytes=mib * 2**20)


def ring_step(value, axis):
    n = lax.axis_size(axis)
    return lax.ppermute(value, axis, [(i, (i + 1) % n) for i in range(n)])


def exchange(value, axis, bit):
    n = lax.axis_size(axis)
    return lax.ppermute(value, axis, [(i, i ^ bit) for i in range(n)])


def later(value, axis, steps):
    n = lax.axis_size(axis)
    return lax.ppermute(value, axis, [(i, i + steps) for i in range(n - steps)])


def plane_gather(chunk):
    half = chunk.shape[0] // 2
    one = exchange(chunk, "fs", 1)
    two = exchange(chunk, "fs", 2)
    return [chunk, one, two, exchange(one[:half], "fs", 2), exchange(two[half:], "fs", 1)]


def line_gather(chunk):
    chunks = [chunk]
    for _ in range(lax.axis_size("sp") - 1):
        chunks.append(ring_step(chunks[-1], "sp"))
    return chunks


def gather_line_first(chunk):
    return plane_gather(jnp.concatenate(line_gather(chunk), axis=0))


def gather_plane_first(chunk):
    return line_gather(jnp.concatenate(plane_gather(chunk), axis=0))


def relative_blocks():
    n_sp, n_fs = lax.axis_size("sp"), lax.axis_size("fs")
    sp, fs = lax.axis_index("sp"), lax.axis_index("fs")
    return jnp.stack(
        [((sp - r) % n_sp) * n_fs + (fs ^ j) for j in range(n_fs) for r in range(n_sp)]
    ).astype(jnp.int32)


def norm_kernel(blocks_ref, x_ref, gain_ref, out_ref):
    width = x_ref.shape[1]
    x = x_ref[...].astype(jnp.float32)
    scale = lax.rsqrt(jnp.sum(x * x, axis=1, keepdims=True) * (1.0 / width) + EPSILON)
    for b in range(width // LANES):
        at = pl.multiple_of(blocks_ref[b] * LANES, LANES)
        part = x_ref[:, pl.ds(at, LANES)].astype(jnp.float32)
        gain = gain_ref[:, pl.ds(at, LANES)]
        out_ref[:, b * LANES : (b + 1) * LANES] = (part * scale * gain).astype(jnp.bfloat16)


def normalise(tokens, gain, blocks):
    rows, width = tokens.shape
    tile = 128
    return pl.pallas_call(
        norm_kernel,
        grid_spec=pltpu.PrefetchScalarGridSpec(
            num_scalar_prefetch=1,
            grid=(rows // tile,),
            in_specs=[
                pl.BlockSpec((tile, width), lambda i, b: (i, 0)),
                pl.BlockSpec((1, width), lambda i, b: (0, 0)),
            ],
            out_specs=pl.BlockSpec((tile, width), lambda i, b: (i, 0)),
        ),
        out_shape=jax.ShapeDtypeStruct((rows, width), jnp.bfloat16),
        name="norm",
    )(blocks, tokens, gain[None, :])


def project_kernel(x_ref, *refs):
    pieces, out_ref = refs[:-1], refs[-1]
    at, total = 0, None
    for piece in pieces:
        depth = piece.shape[0]
        part = jnp.dot(x_ref[:, at : at + depth], piece[...], preferred_element_type=jnp.float32)
        total = part if total is None else total + part
        at += depth
    out_ref[...] = total.astype(jnp.bfloat16)


def project(normed, pieces):
    rows, depth = normed.shape
    cols = pieces[0].shape[1]
    tile = 256
    return pl.pallas_call(
        project_kernel,
        grid=(cols // tile,),
        in_specs=[pl.BlockSpec((rows, depth), lambda i: (0, 0))]
        + [pl.BlockSpec((p.shape[0], tile), lambda i: (0, i)) for p in pieces],
        out_specs=pl.BlockSpec((rows, tile), lambda i: (0, i)),
        out_shape=jax.ShapeDtypeStruct((rows, cols), jnp.bfloat16),
        compiler_params=vmem(48),
        cost_estimate=pl.CostEstimate(
            flops=2 * rows * depth * cols, bytes_accessed=2 * depth * (rows + cols), transcendentals=0
        ),
        name="project",
    )(normed, *pieces)


def output_kernel(place_ref, ret_ref, conv_ref, *refs):
    pieces, out_ref = refs[:-1], refs[-1]
    n_fs = place_ref[3]
    split = ret_ref.shape[1]
    for r, piece in enumerate(pieces):
        dims = (((1,), (1,)), ((), ()))
        part = lax.dot_general(
            ret_ref[...], piece[:, :split], dims, preferred_element_type=jnp.float32
        ) + lax.dot_general(
            conv_ref[...], piece[:, split:], dims, preferred_element_type=jnp.float32
        )
        part = part.astype(jnp.bfloat16)
        base = lax.rem(place_ref[1] - r + len(pieces), len(pieces)) * n_fs
        for j in range(part.shape[1] // LANES):
            at = pl.multiple_of((base + (place_ref[2] ^ j)) * LANES, LANES)
            out_ref[:, pl.ds(at, LANES)] = part[:, j * LANES : (j + 1) * LANES]


def output_rows(ret_out, conv_out, pieces, place):
    rows = ret_out.shape[0] // 2
    tile = rows // 2 if rows % 32 == 0 else rows
    steps = rows // tile
    width = sum(p.shape[0] for p in pieces)
    acts = [
        pl.BlockSpec((tile, a.shape[1]), lambda i, s: (s[0] * steps + i, 0))
        for a in (ret_out, conv_out)
    ]
    return pl.pallas_call(
        output_kernel,
        grid_spec=pltpu.PrefetchScalarGridSpec(
            num_scalar_prefetch=1,
            grid=(steps,),
            in_specs=acts + [pl.BlockSpec(p.shape, lambda i, s: (0, 0)) for p in pieces],
            out_specs=pl.BlockSpec((tile, width), lambda i, s: (i, 0)),
        ),
        out_shape=jax.ShapeDtypeStruct((rows, width), jnp.bfloat16),
        compiler_params=vmem(48),
        name="output",
    )(place, ret_out, conv_out, *pieces)


def rotate(values, token_ordinal):
    half_dim = values.shape[-1] // 2
    frequency = 1.0 / ROPE_BASE ** jnp.linspace(0.0, 1.0, half_dim, dtype=jnp.float32)
    angles = token_ordinal[:, None] * frequency[None, :]
    cosine_table = jnp.cos(angles)[:, None, :]
    sine_table = jnp.sin(angles)[:, None, :]
    first = values[..., :half_dim].astype(jnp.float32)
    second = values[..., half_dim:].astype(jnp.float32)
    return jnp.concatenate(
        [first * cosine_table - second * sine_table, first * sine_table + second * cosine_table],
        axis=-1,
    )


def retention_local(projections, decays, token_ordinal):
    tok_rows = token_ordinal.shape[0]
    head_count = decays.shape[0]
    blocks = tok_rows // BLOCK_LEN
    query_raw = projections[0].reshape(tok_rows, head_count, KEY_DIM)
    key_raw = projections[1].reshape(tok_rows, head_count, KEY_DIM)
    queries = rotate(query_raw, token_ordinal).astype(jnp.bfloat16)
    keys = (rotate(key_raw, token_ordinal) * KEY_DIM ** (-0.5)).astype(jnp.bfloat16)
    value_proj = projections[2].reshape(tok_rows, head_count, VALUE_DIM)

    def split_blocks(array):
        shaped = array.reshape(blocks, BLOCK_LEN, head_count, array.shape[-1])
        return jnp.transpose(shaped, (0, 2, 1, 3))

    query_blocks = split_blocks(queries)
    key_blocks = split_blocks(keys)
    value_blocks = split_blocks(value_proj)
    decay_blocks = jnp.transpose(decays.reshape(head_count, blocks, BLOCK_LEN), (1, 0, 2))
    cumulative = jnp.cumsum(decay_blocks, axis=-1)
    ending = cumulative[..., -1:]
    decay_gaps = cumulative[..., :, None] - cumulative[..., None, :]
    causal = jnp.arange(BLOCK_LEN)[:, None] >= jnp.arange(BLOCK_LEN)[None, :]
    weighting = jnp.where(causal, jnp.exp(jnp.minimum(decay_gaps, 0.0)), 0.0)
    raw_scores = jnp.einsum(
        "nhid,nhjd->nhij", query_blocks, key_blocks, preferred_element_type=jnp.float32
    )
    scores = (raw_scores * weighting).astype(jnp.bfloat16)
    intra_out = jnp.einsum(
        "nhij,nhje->nhie", scores, value_blocks, preferred_element_type=jnp.float32
    )
    decayed_keys = (
        key_blocks.astype(jnp.float32) * jnp.exp(ending - cumulative)[..., None]
    ).astype(jnp.bfloat16)
    decayed_queries = (query_blocks.astype(jnp.float32) * jnp.exp(cumulative)[..., None]).astype(
        jnp.bfloat16
    )
    block_kv = jnp.einsum(
        "nhjd,nhje->nhde", decayed_keys, value_blocks, preferred_element_type=jnp.float32
    )
    block_ends = ending[..., 0]
    state = jnp.zeros((head_count, KEY_DIM, VALUE_DIM), jnp.float32)
    before = []
    for n in range(blocks):
        before.append(state)
        state = state * jnp.exp(block_ends[n])[:, None, None] + block_kv[n]
    device_total = jnp.sum(block_ends, axis=0)
    return (intra_out, decayed_queries, jnp.stack(before), block_ends, state, device_total)


def state_before(end_state, device_total):
    n = lax.axis_size("sp")
    high = device_total.astype(jnp.bfloat16)
    low = (device_total - high.astype(jnp.float32)).astype(jnp.bfloat16)
    wide = (device_total.shape[0], 8, VALUE_DIM)
    message = jnp.concatenate(
        [
            end_state.astype(jnp.bfloat16),
            jnp.broadcast_to(high[:, None, None], wide),
            jnp.broadcast_to(low[:, None, None], wide),
        ],
        axis=1,
    )
    total, decay = None, None
    for k in range(1, n):
        got = later(message, "sp", k).astype(jnp.float32)
        state = got[:, :KEY_DIM]
        log = got[:, KEY_DIM, :1] + got[:, KEY_DIM + 8, :1]
        if k == 1:
            total, decay = state, log
        else:
            total = total + jnp.exp(decay)[:, :, None] * state
            decay = decay + log
    return total


def retention_finish(local_parts, state_in):
    intra_out, decayed_queries, before_local, block_ends, _, _ = local_parts
    starts = jnp.cumsum(block_ends, axis=0) - block_ends
    full_states = before_local + jnp.exp(starts)[:, :, None, None] * state_in[None]
    cross = jnp.einsum(
        "nhid,nhde->nhie",
        decayed_queries,
        full_states.astype(jnp.bfloat16),
        preferred_element_type=jnp.float32,
    )
    output = intra_out + cross
    output = output * lax.rsqrt(jnp.mean(output * output, axis=-1, keepdims=True) + EPSILON)
    blocks, heads = output.shape[:2]
    return jnp.transpose(output, (0, 2, 1, 3)).reshape(blocks * BLOCK_LEN, heads * VALUE_DIM)


def convolved(gate_c, conv_input, conv_kernel):
    tok_rows = gate_c.shape[0]
    product = gate_c.astype(jnp.float32) * conv_input.astype(jnp.float32)
    rim_rows = later(product[tok_rows - (CONV_TAPS - 1) :], "sp", 1)
    padded = jnp.concatenate([rim_rows, product], axis=0)
    out = jnp.zeros_like(product)
    for tap_index in range(CONV_TAPS):
        out = out + conv_kernel[tap_index] * padded[tap_index : tap_index + tok_rows]
    return out


def shards(
    tokens,
    norm_gain,
    query_weight,
    key_weight,
    value_weight,
    gate_weight,
    conv_b_weight,
    conv_c_weight,
    conv_in_weight,
    conv_kernel,
    out_ret_weight,
    out_conv_weight,
    log_decay,
):
    tok_rows = tokens.shape[1]
    key_cols, value_cols = query_weight.shape[1], value_weight.shape[1]
    conv_cols = conv_c_weight.shape[1]

    def side_by_side(*arrays):
        return jnp.concatenate(arrays, axis=1)

    out_pieces = gather_plane_first(side_by_side(out_ret_weight, out_conv_weight))
    qkv_pieces = gather_line_first(side_by_side(query_weight, key_weight, value_weight))
    ci_pieces = gather_line_first(side_by_side(conv_c_weight, conv_in_weight))
    gb_pieces = gather_line_first(side_by_side(gate_weight, conv_b_weight))

    normed = normalise(tokens[0], norm_gain, relative_blocks())
    token_ordinal = (
        lax.axis_index("sp") * tok_rows + jnp.arange(tok_rows, dtype=jnp.int32)
    ).astype(jnp.float32)

    qkv = project(normed, qkv_pieces)
    local_parts = retention_local(
        (qkv[:, :key_cols], qkv[:, key_cols : 2 * key_cols], qkv[:, 2 * key_cols :]),
        log_decay[0],
        token_ordinal,
    )
    state_in = state_before(local_parts[4], local_parts[5])
    ci = project(normed, ci_pieces)
    conv = convolved(ci[:, :conv_cols], ci[:, conv_cols:], conv_kernel)
    retained = retention_finish(local_parts, state_in)

    gb = project(normed, gb_pieces)
    ret_out = (retained * jax.nn.silu(gb[:, :value_cols].astype(jnp.float32))).astype(jnp.bfloat16)
    conv_out = (gb[:, value_cols:].astype(jnp.float32) * conv).astype(jnp.bfloat16)

    tp = lax.axis_index("tp")
    sp, fs = lax.axis_index("sp"), lax.axis_index("fs")

    def place(half):
        return jnp.stack([half, sp, fs, jnp.int32(lax.axis_size("fs"))]).astype(jnp.int32)

    theirs = output_rows(ret_out, conv_out, out_pieces, place(1 - tp))
    received = exchange(theirs, "tp", 1)
    mine = output_rows(ret_out, conv_out, out_pieces, place(tp))
    mixed = (mine.astype(jnp.float32) + received.astype(jnp.float32)).astype(jnp.bfloat16)
    return mixed[None]


def shards_plain(
    tokens,
    norm_gain,
    query_weight,
    key_weight,
    value_weight,
    gate_weight,
    conv_b_weight,
    conv_c_weight,
    conv_in_weight,
    conv_kernel,
    out_ret_weight,
    out_conv_weight,
    log_decay,
):
    tok_rows = tokens.shape[1]
    key_cols, value_cols = query_weight.shape[1], value_weight.shape[1]
    x = tokens[0].astype(jnp.float32)
    normed = x * lax.rsqrt(jnp.mean(x * x, axis=-1, keepdims=True) + EPSILON) * norm_gain
    normed = normed.astype(jnp.bfloat16)
    token_ordinal = (
        lax.axis_index("sp") * tok_rows + jnp.arange(tok_rows, dtype=jnp.int32)
    ).astype(jnp.float32)

    def whole(*weights):
        return lax.all_gather(
            jnp.concatenate(weights, axis=1), ("sp", "fs"), axis=0, tiled=True
        )

    def apply(*weights):
        full = jnp.dot(normed, whole(*weights), preferred_element_type=jnp.float32)
        return full.astype(jnp.bfloat16)

    qkv = apply(query_weight, key_weight, value_weight)
    local_parts = retention_local(
        (qkv[:, :key_cols], qkv[:, key_cols : 2 * key_cols], qkv[:, 2 * key_cols :]),
        log_decay[0],
        token_ordinal,
    )
    state_in = state_before(local_parts[4], local_parts[5])
    ci = apply(conv_c_weight, conv_in_weight)
    conv = convolved(ci[:, : ci.shape[1] // 2], ci[:, ci.shape[1] // 2 :], conv_kernel)
    retained = retention_finish(local_parts, state_in)
    gb = apply(gate_weight, conv_b_weight)
    ret_out = (retained * jax.nn.silu(gb[:, :value_cols].astype(jnp.float32))).astype(jnp.bfloat16)
    conv_out = (gb[:, value_cols:].astype(jnp.float32) * conv).astype(jnp.bfloat16)
    partial = lax.dot_general(
        jnp.concatenate([ret_out, conv_out], axis=1),
        whole(out_ret_weight, out_conv_weight),
        (((1,), (1,)), ((), ())),
        preferred_element_type=jnp.float32,
    )
    mixed = lax.psum_scatter(
        partial.astype(jnp.bfloat16), "tp", scatter_dimension=0, tiled=True
    )
    return mixed[None]


def local_layer(*arrays):
    rows, model = arrays[2].shape[0], arrays[0].shape[2]
    sizes = [a.shape[1] for a in arrays[2:9]]
    fits = (
        rows % LANES == 0
        and all(size % LANES == 0 for size in sizes)
        and lax.axis_size("fs") == 4
        and lax.axis_size("tp") == 2
        and model == rows * 4 * lax.axis_size("sp")
    )
    return (shards if fits else shards_plain)(*arrays)


def solution(mesh):
    rows = P(("sp", "fs"), "tp")
    in_specs = (P("fs", "sp", None), P()) + (rows,) * 7 + (P(None, "tp"), rows, rows, P("fs", "tp", "sp"))
    out_specs = P("fs", ("sp", "tp"), None)
    return jax.shard_map(local_layer, mesh=mesh, in_specs=in_specs, out_specs=out_specs, check_vma=False)
```

```python
import functools

import jax
import jax.numpy as jnp
import numpy as np
from jax import lax
from jax.experimental import pallas as pl
from jax.experimental.pallas import tpu as pltpu
from jax.sharding import PartitionSpec as P


KEY_DIM = 64
VALUE_DIM = 128
CONV_TAPS = 3
BLOCK_LEN = 128
LANES = 128

EPSILON = 1e-06
ROPE_BASE = 10000.0


DOT_ROWS = (((1,), (1,)), ((), ()))


def vmem(mib):
    return pltpu.CompilerParams(vmem_limit_bytes=mib * 2**20)


def ring_step(value, axis):
    n = lax.axis_size(axis)
    return lax.ppermute(value, axis, [(i, (i + 1) % n) for i in range(n)])


def exchange(value, axis, bit):
    n = lax.axis_size(axis)
    return lax.ppermute(value, axis, [(i, i ^ bit) for i in range(n)])


def later(value, axis, steps):
    n = lax.axis_size(axis)
    return lax.ppermute(value, axis, [(i, i + steps) for i in range(n - steps)])


def line_gather(chunk):
    chunks = [chunk]
    for _ in range(1, lax.axis_size("sp")):
        chunks.append(ring_step(chunks[-1], "sp"))
    return chunks


def gather_line_first(chunk):
    chunks = line_gather(chunk)
    half = len(chunks) // 2
    pieces = []
    for part, group in (("a", chunks[:half]), ("b", chunks[half:])):
        own = jnp.concatenate(group, axis=0)
        one = exchange(own, "fs", 1)
        two = exchange(own, "fs", 2)
        if part == "a":
            three = exchange(one, "fs", 2)
        else:
            three = exchange(two, "fs", 1)
        pieces += [own, one, two, three]
    return pieces


def gather_plane_first(chunk):
    half = chunk.shape[0] // 2
    one = exchange(chunk, "fs", 1)
    two = exchange(chunk, "fs", 2)
    three = [exchange(one[:half], "fs", 2), exchange(two[half:], "fs", 1)]
    return line_gather(jnp.concatenate([chunk, one, two] + three, axis=0))


def relative_blocks():
    n_sp, n_fs = lax.axis_size("sp"), lax.axis_size("fs")
    sp, fs = lax.axis_index("sp"), lax.axis_index("fs")
    half = n_sp // 2
    order = [
        (r, j)
        for group in (range(half), range(half, n_sp))
        for j in range(n_fs)
        for r in group
    ]
    return jnp.stack([((sp - r) % n_sp) * n_fs + (fs ^ j) for r, j in order]).astype(jnp.int32)


def norm_kernel(blocks_ref, x_ref, gain_ref, out_ref):
    width = x_ref.shape[1]
    x = x_ref[...].astype(jnp.float32)
    scale = lax.rsqrt(jnp.sum(x * x, axis=1, keepdims=True) * (1.0 / width) + EPSILON)
    for b in range(width // LANES):
        at = pl.multiple_of(blocks_ref[b] * LANES, LANES)
        part = x_ref[:, pl.ds(at, LANES)].astype(jnp.float32)
        gain = gain_ref[:, pl.ds(at, LANES)]
        out_ref[:, b * LANES : (b + 1) * LANES] = (part * scale * gain).astype(jnp.bfloat16)


def normalise(tokens, gain, blocks):
    rows, width = tokens.shape
    tile = 128
    return pl.pallas_call(
        norm_kernel,
        grid_spec=pltpu.PrefetchScalarGridSpec(
            num_scalar_prefetch=1,
            grid=(rows // tile,),
            in_specs=[
                pl.BlockSpec((tile, width), lambda i, b: (i, 0)),
                pl.BlockSpec((1, width), lambda i, b: (0, 0)),
            ],
            out_specs=pl.BlockSpec((tile, width), lambda i, b: (i, 0)),
        ),
        out_shape=jax.ShapeDtypeStruct((rows, width), jnp.bfloat16),
        name="norm",
    )(blocks, *in_hbm(tokens), gain[None, :])


def in_hbm(*arrays):
    return [pltpu.with_memory_space_constraint(a, pltpu.HBM) for a in arrays]


def pack_kernel(groups, *refs):
    ins, outs = refs[: sum(groups)], refs[sum(groups) :]
    taken = 0
    for out, count in zip(outs, groups):
        at = 0
        for ref in ins[taken : taken + count]:
            out[:, at : at + ref.shape[1]] = ref[...]
            at += ref.shape[1]
        taken += count


def pack(*groups):
    arrays = [w for group in groups for w in group]
    rows = arrays[0].shape[0]
    widths = [sum(w.shape[1] for w in group) for group in groups]
    return pl.pallas_call(
        functools.partial(pack_kernel, [len(group) for group in groups]),
        grid=(1,),
        in_specs=[pl.BlockSpec(w.shape, lambda i: (0, 0)) for w in arrays],
        out_specs=[pl.BlockSpec((rows, w), lambda i: (0, 0)) for w in widths],
        out_shape=[jax.ShapeDtypeStruct((rows, w), jnp.bfloat16) for w in widths],
        compiler_params=vmem(8),
        name="pack",
    )(*in_hbm(*arrays))


def joined(pieces):
    return jnp.concatenate([piece[...] for piece in pieces], axis=0)


def product(x, weights):
    return jnp.dot(x, weights, preferred_element_type=jnp.float32)


def rounded(x):
    return x.astype(jnp.bfloat16).astype(jnp.float32)


def cost(rows, depth, cols):
    return pl.CostEstimate(
        flops=2 * rows * depth * cols, bytes_accessed=2 * depth * (rows + cols), transcendentals=0
    )


def project_kernel(x_ref, *refs):
    pieces, out_ref = refs[:-1], refs[-1]
    out_ref[...] = product(x_ref[...], joined(pieces)).astype(jnp.bfloat16)


def project(normed, pieces):
    rows, depth = normed.shape
    cols = pieces[0].shape[1]
    tile = 256
    return pl.pallas_call(
        project_kernel,
        grid=(cols // tile,),
        in_specs=[pl.BlockSpec(memory_space=pltpu.VMEM)]
        + [pl.BlockSpec((p.shape[0], tile), lambda i: (0, i)) for p in pieces],
        out_specs=pl.BlockSpec((rows, tile), lambda i: (0, i)),
        out_shape=jax.ShapeDtypeStruct((rows, cols), jnp.bfloat16),
        compiler_params=vmem(24),
        cost_estimate=cost(rows, depth, cols),
        name="project",
    )(normed, *in_hbm(*pieces))


def conv_kernel_body(x_ref, taps_ref, *refs):
    pieces, (out_ref, rim_ref) = refs[:-2], refs[-2:]
    half = len(pieces) // 2
    x = x_ref[...]
    gate = rounded(product(x, joined(pieces[:half])))
    value = rounded(product(x, joined(pieces[half:])))
    gated = gate * value
    rows = gated.shape[0]
    row = lax.broadcasted_iota(jnp.int32, gated.shape, 0)
    total = taps_ref[CONV_TAPS - 1 : CONV_TAPS, :] * gated
    for back in range(1, CONV_TAPS):
        moved = jnp.where(row >= back, pltpu.roll(gated, back, axis=0), 0.0)
        tap = CONV_TAPS - 1 - back
        total = total + taps_ref[tap : tap + 1, :] * moved
    out_ref[...] = total
    rim_ref[...] = gated[rows - 8 :, :]


def conv_local(normed, pieces, taps):
    rows, depth = normed.shape
    cols = pieces[0].shape[1] // 2
    tile = 256
    steps = cols // tile
    return pl.pallas_call(
        conv_kernel_body,
        grid=(steps,),
        in_specs=[
            pl.BlockSpec(memory_space=pltpu.VMEM),
            pl.BlockSpec((CONV_TAPS, tile), lambda i: (0, i)),
        ]
        + [pl.BlockSpec((p.shape[0], tile), lambda i: (0, i)) for p in pieces]
        + [pl.BlockSpec((p.shape[0], tile), lambda i: (0, i + steps)) for p in pieces],
        out_specs=[
            pl.BlockSpec((rows, tile), lambda i: (0, i)),
            pl.BlockSpec((8, tile), lambda i: (0, i)),
        ],
        out_shape=[
            pltpu.HBM((rows, cols), jnp.float32),
            jax.ShapeDtypeStruct((8, cols), jnp.float32),
        ],
        compiler_params=vmem(24),
        cost_estimate=cost(rows, depth, 2 * cols),
        name="conv",
    )(normed, taps, *in_hbm(*pieces), *in_hbm(*pieces))


def retention_kernel(
    place_ref, decay_ref, q_ref, k_ref, v_ref, turn_ref, base_ref, y_ref, dq_ref, message_ref
):
    rows = q_ref.shape[0]
    blocks = rows // BLOCK_LEN
    shape = (BLOCK_LEN, LANES)
    lane = lax.broadcasted_iota(jnp.int32, shape, 1)
    first_half = lane % KEY_DIM < KEY_DIM // 2
    causal = lax.broadcasted_iota(jnp.int32, shape, 0) >= lane
    upto = jnp.where(causal, 1.0, 0.0)
    heads = LANES // KEY_DIM
    own = [lane // KEY_DIM == h for h in range(heads)]
    exact = dict(precision=lax.Precision.HIGHEST, preferred_element_type=jnp.float32)
    states = [None] * heads
    start = jnp.zeros((1, heads), jnp.float32)
    for n in range(blocks):
        at = slice(n * BLOCK_LEN, (n + 1) * BLOCK_LEN)
        line = pl.ds(place_ref[1] * blocks + n, 1)
        within, base = (turn_ref[0], turn_ref[1]), (base_ref[0, line, :], base_ref[1, line, :])
        cosine = within[0] * base[0] - within[1] * base[1]
        sine = within[1] * base[0] + within[0] * base[1]
        sine = jnp.where(first_half, -sine, sine)

        def turned(ref):
            x = ref[at, :].astype(jnp.float32)
            swapped = jnp.where(
                first_half,
                pltpu.roll(x, LANES - KEY_DIM // 2, axis=1),
                pltpu.roll(x, KEY_DIM // 2, axis=1),
            )
            return x * cosine + swapped * sine

        queries = turned(q_ref).astype(jnp.bfloat16)
        keys = (turned(k_ref) * KEY_DIM ** (-0.5)).astype(jnp.bfloat16)
        q32, k32 = queries.astype(jnp.float32), keys.astype(jnp.float32)
        decays = decay_ref[0, :, at]
        cols = lax.dot_general(upto, decays, DOT_ROWS, **exact)
        lines = lax.dot_general(decays, upto, DOT_ROWS, **exact)
        ends = cols[BLOCK_LEN - 1 :, :]
        from_start = None
        for h in range(heads):
            col, row, end = cols[:, h : h + 1], lines[h : h + 1, :], ends[:, h : h + 1]
            weights = jnp.where(causal, jnp.exp(jnp.minimum(col - row, 0.0)), 0.0)
            mine = jnp.where(own[h], q32, 0.0)
            raw = lax.dot_general(
                mine.astype(jnp.bfloat16), keys, DOT_ROWS, preferred_element_type=jnp.float32
            )
            values = v_ref[at, h * VALUE_DIM : (h + 1) * VALUE_DIM]
            out = product((raw * weights).astype(jnp.bfloat16), values)
            if n:
                decayed = (mine * jnp.exp(col)).astype(jnp.bfloat16)
                out = out + product(decayed, states[h].astype(jnp.bfloat16))
            y_ref[at, h * VALUE_DIM : (h + 1) * VALUE_DIM] = out
            decayed = jnp.where(own[h], k32 * jnp.exp(end - col), 0.0).astype(jnp.bfloat16)
            block = lax.dot_general(
                decayed, values, (((0,), (0,)), ((), ())), preferred_element_type=jnp.float32
            )
            if n:
                block = block + states[h] * jnp.exp(end)
            states[h] = block
            part = mine * jnp.exp(col + start[:, h : h + 1])
            from_start = part if from_start is None else from_start + part
        dq_ref[at, :] = from_start.astype(jnp.bfloat16)
        start = start + ends
    total = states[0]
    for h in range(1, heads):
        total = total + states[h]
    message_ref[0:LANES, :] = total.astype(jnp.bfloat16)
    logs = []
    for h in range(heads):
        log = jnp.broadcast_to(start[:, h : h + 1], (1, VALUE_DIM))
        high = log.astype(jnp.bfloat16).astype(jnp.float32)
        logs += [high, log - high]
    spare = jnp.zeros((16 - len(logs), VALUE_DIM), jnp.float32)
    message_ref[LANES:, :] = jnp.concatenate(logs + [spare], axis=0).astype(jnp.bfloat16)


def turns(positions):
    half_dim = KEY_DIM // 2
    frequency = ROPE_BASE ** -np.linspace(0.0, 1.0, half_dim)
    angles = np.tile(positions[:, None] * frequency[None, :], (1, LANES // half_dim))
    return jnp.asarray(np.stack([np.cos(angles), np.sin(angles)]), jnp.float32)


def retention(qkv, decays, place):
    rows = qkv.shape[0]
    heads = decays.shape[0]
    pairs = heads * KEY_DIM // LANES
    per = heads // pairs
    values = qkv.shape[1] - 2 * heads * KEY_DIM
    within = turns(np.arange(BLOCK_LEN))
    base = turns(np.arange(0, rows * lax.axis_size("sp"), BLOCK_LEN))
    wide = per * VALUE_DIM
    skip = 2 * heads * KEY_DIM
    return pl.pallas_call(
        retention_kernel,
        grid_spec=pltpu.PrefetchScalarGridSpec(
            num_scalar_prefetch=1,
            grid=(pairs,),
            in_specs=[
                pl.BlockSpec((1, per, rows), lambda p, s: (p, 0, 0)),
                pl.BlockSpec((rows, LANES), lambda p, s: (0, p)),
                pl.BlockSpec((rows, LANES), lambda p, s: (0, p + pairs)),
                pl.BlockSpec((rows, wide), lambda p, s: (0, p + skip // wide)),
                pl.BlockSpec(within.shape, lambda p, s: (0, 0, 0)),
                pl.BlockSpec(base.shape, lambda p, s: (0, 0, 0)),
            ],
            out_specs=[
                pl.BlockSpec((rows, wide), lambda p, s: (0, p)),
                pl.BlockSpec((rows, LANES), lambda p, s: (0, p)),
                pl.BlockSpec((LANES + 16, VALUE_DIM), lambda p, s: (p, 0)),
            ],
        ),
        out_shape=[
            pltpu.HBM((rows, values), jnp.float32),
            pltpu.HBM((rows, heads * KEY_DIM), jnp.bfloat16),
            jax.ShapeDtypeStruct((pairs * (LANES + 16), VALUE_DIM), jnp.bfloat16),
        ],
        compiler_params=vmem(16),
        name="retention",
    )(place, decays.reshape(pairs, per, rows), qkv, qkv, qkv, within, base)


def gate_kernel(count, place_ref, x_ref, y_ref, dq_ref, conv_ref, rim_ref, taps_ref, *refs):
    earlier, pieces, (mine_ref, theirs_ref, act_ref) = refs[:count], refs[count:-3], refs[-3:]
    gate = rounded(product(x_ref[...], joined(pieces)))
    step = pl.program_id(0)

    @pl.when(step < pl.num_programs(0) // 2)
    def _():
        lines = lax.broadcasted_iota(jnp.int32, (LANES, VALUE_DIM), 0)
        for h in range(LANES // KEY_DIM):
            at = slice(h * VALUE_DIM, (h + 1) * VALUE_DIM)
            state, decay = None, None
            for ref in earlier:
                before = ref[0:LANES, :].astype(jnp.float32)
                logs = ref[LANES:, :].astype(jnp.float32)
                log = logs[2 * h : 2 * h + 1] + logs[2 * h + 1 : 2 * h + 2]
                state = before if state is None else state + jnp.exp(decay) * before
                decay = log if decay is None else decay + log
            state = jnp.where(lines // KEY_DIM == h, state, 0.0).astype(jnp.bfloat16)
            y = y_ref[:, at] + product(dq_ref[...], state)
            y = y * lax.rsqrt(jnp.mean(y * y, axis=1, keepdims=True) + EPSILON)
            g = gate[:, at]
            act_ref[:, at] = (y * (g / (1.0 + jnp.exp(-g)))).astype(jnp.bfloat16)

    @pl.when(step >= pl.num_programs(0) // 2)
    def _():
        act_ref[...] = (gate * conv_ref[...]).astype(jnp.bfloat16)
        last, before = rim_ref[1:2, :], rim_ref[0:1, :]
        row = lax.broadcasted_iota(jnp.int32, (16, gate.shape[1]), 0)
        extra = jnp.where(
            row == 0,
            taps_ref[0:1, :] * before + taps_ref[1:2, :] * last,
            jnp.where(row == 1, taps_ref[0:1, :] * last, 0.0),
        )
        act_ref[0:16, :] = (gate[0:16, :] * (conv_ref[0:16, :] + extra)).astype(jnp.bfloat16)

    half = mine_ref.shape[0]
    own = place_ref[0] * half
    mine_ref[...] = act_ref[pl.ds(pl.multiple_of(own, 16), half), :]
    theirs_ref[...] = act_ref[pl.ds(pl.multiple_of(half - own, 16), half), :]


def gated(normed, pieces, y, dq, earlier, conv, rim, taps, place):
    rows, depth = normed.shape
    cols = pieces[0].shape[1]
    tile = VALUE_DIM * LANES // KEY_DIM
    split = y.shape[1] // tile
    head = lambda i, s: (0, jnp.minimum(i, split - 1))
    chan = lambda i, s: (0, jnp.maximum(i - split, 0))
    out = jax.ShapeDtypeStruct((rows // 2, cols), jnp.bfloat16)
    return pl.pallas_call(
        functools.partial(gate_kernel, len(earlier)),
        grid_spec=pltpu.PrefetchScalarGridSpec(
            num_scalar_prefetch=1,
            grid=(cols // tile,),
            in_specs=[
                pl.BlockSpec(memory_space=pltpu.VMEM),
                pl.BlockSpec((rows, tile), head),
                pl.BlockSpec((rows, LANES), head),
                pl.BlockSpec((rows, tile), chan),
                pl.BlockSpec((rim.shape[0], tile), chan),
                pl.BlockSpec((CONV_TAPS, tile), chan),
            ]
            + [pl.BlockSpec((LANES + 16, VALUE_DIM), lambda i, s: head(i, s)[::-1]) for _ in earlier]
            + [pl.BlockSpec((p.shape[0], tile), lambda i, s: (0, i)) for p in pieces],
            out_specs=[pl.BlockSpec((rows // 2, tile), lambda i, s: (0, i))] * 2,
            scratch_shapes=[pltpu.VMEM((rows, tile), jnp.bfloat16)],
        ),
        out_shape=[out, out],
        compiler_params=vmem(24),
        cost_estimate=cost(rows, depth, cols),
        name="gate",
    )(place, normed, *in_hbm(y, dq, conv), rim, taps, *earlier, *in_hbm(*pieces))


def part_kernel(act_ref, *refs):
    pieces, out_ref = refs[:-1], refs[-1]
    at = 0
    for piece in pieces:
        part = lax.dot_general(
            act_ref[...], piece[...], DOT_ROWS, preferred_element_type=jnp.float32
        )
        out_ref[:, at : at + part.shape[1]] = part.astype(jnp.bfloat16)
        at += part.shape[1]


def output_part(acts, pieces):
    rows = acts.shape[0]
    width = sum(p.shape[0] for p in pieces)
    return pl.pallas_call(
        part_kernel,
        grid=(1,),
        in_specs=[pl.BlockSpec(acts.shape, lambda i: (0, 0))]
        + [pl.BlockSpec(memory_space=pltpu.VMEM)] * len(pieces),
        out_specs=pl.BlockSpec((rows, width), lambda i: (0, 0)),
        out_shape=jax.ShapeDtypeStruct((rows, width), jnp.bfloat16),
        compiler_params=vmem(16),
        cost_estimate=cost(rows, acts.shape[1], width),
        name="part",
    )(acts, *pieces)


def merge_kernel(n_sp, place_ref, *refs):
    parts, out_ref = refs[:-1], refs[-1]
    n_fs = place_ref[3]
    block = 0
    for one, two in zip(parts[::2], parts[1::2]):
        for at in range(0, one.shape[1], LANES):
            cols = slice(at, at + LANES)
            total = one[:, cols].astype(jnp.float32) + two[:, cols].astype(jnp.float32)
            r, j = lax.div(block, n_fs), lax.rem(block, n_fs)
            base = lax.rem(place_ref[1] - r + n_sp, n_sp) * n_fs
            to = pl.multiple_of((base + (place_ref[2] ^ j)) * LANES, LANES)
            out_ref[:, pl.ds(to, LANES)] = total.astype(jnp.bfloat16)
            block += 1


def merged(parts, place):
    rows = parts[0].shape[0]
    width = sum(p.shape[1] for p in parts[::2])
    tile = rows // 2
    return pl.pallas_call(
        functools.partial(merge_kernel, lax.axis_size("sp")),
        grid_spec=pltpu.PrefetchScalarGridSpec(
            num_scalar_prefetch=1,
            grid=(rows // tile,),
            in_specs=[pl.BlockSpec((tile, p.shape[1]), lambda i, s: (i, 0)) for p in parts],
            out_specs=pl.BlockSpec((tile, width), lambda i, s: (i, 0)),
        ),
        out_shape=jax.ShapeDtypeStruct((rows, width), jnp.bfloat16),
        compiler_params=vmem(16),
        name="merge",
    )(place, *parts)


def rotate(values, token_ordinal):
    half_dim = values.shape[-1] // 2
    frequency = 1.0 / ROPE_BASE ** jnp.linspace(0.0, 1.0, half_dim, dtype=jnp.float32)
    angles = token_ordinal[:, None] * frequency[None, :]
    cosine_table = jnp.cos(angles)[:, None, :]
    sine_table = jnp.sin(angles)[:, None, :]
    first = values[..., :half_dim].astype(jnp.float32)
    second = values[..., half_dim:].astype(jnp.float32)
    return jnp.concatenate(
        [first * cosine_table - second * sine_table, first * sine_table + second * cosine_table],
        axis=-1,
    )


def retention_local(projections, decays, token_ordinal):
    tok_rows = token_ordinal.shape[0]
    head_count = decays.shape[0]
    blocks = tok_rows // BLOCK_LEN
    query_raw = projections[0].reshape(tok_rows, head_count, KEY_DIM)
    key_raw = projections[1].reshape(tok_rows, head_count, KEY_DIM)
    queries = rotate(query_raw, token_ordinal).astype(jnp.bfloat16)
    keys = (rotate(key_raw, token_ordinal) * KEY_DIM ** (-0.5)).astype(jnp.bfloat16)
    value_proj = projections[2].reshape(tok_rows, head_count, VALUE_DIM)

    def split_blocks(array):
        shaped = array.reshape(blocks, BLOCK_LEN, head_count, array.shape[-1])
        return jnp.transpose(shaped, (0, 2, 1, 3))

    query_blocks = split_blocks(queries)
    key_blocks = split_blocks(keys)
    value_blocks = split_blocks(value_proj)
    decay_blocks = jnp.transpose(decays.reshape(head_count, blocks, BLOCK_LEN), (1, 0, 2))
    cumulative = jnp.cumsum(decay_blocks, axis=-1)
    ending = cumulative[..., -1:]
    decay_gaps = cumulative[..., :, None] - cumulative[..., None, :]
    causal = jnp.arange(BLOCK_LEN)[:, None] >= jnp.arange(BLOCK_LEN)[None, :]
    weighting = jnp.where(causal, jnp.exp(jnp.minimum(decay_gaps, 0.0)), 0.0)
    raw_scores = jnp.einsum(
        "nhid,nhjd->nhij", query_blocks, key_blocks, preferred_element_type=jnp.float32
    )
    scores = (raw_scores * weighting).astype(jnp.bfloat16)
    intra_out = jnp.einsum(
        "nhij,nhje->nhie", scores, value_blocks, preferred_element_type=jnp.float32
    )
    decayed_keys = (
        key_blocks.astype(jnp.float32) * jnp.exp(ending - cumulative)[..., None]
    ).astype(jnp.bfloat16)
    decayed_queries = (query_blocks.astype(jnp.float32) * jnp.exp(cumulative)[..., None]).astype(
        jnp.bfloat16
    )
    block_kv = jnp.einsum(
        "nhjd,nhje->nhde", decayed_keys, value_blocks, preferred_element_type=jnp.float32
    )
    block_ends = ending[..., 0]
    state = jnp.zeros((head_count, KEY_DIM, VALUE_DIM), jnp.float32)
    before = []
    for n in range(blocks):
        before.append(state)
        state = state * jnp.exp(block_ends[n])[:, None, None] + block_kv[n]
    device_total = jnp.sum(block_ends, axis=0)
    return (intra_out, decayed_queries, jnp.stack(before), block_ends, state, device_total)


def state_before(end_state, device_total):
    n = lax.axis_size("sp")
    high = device_total.astype(jnp.bfloat16)
    low = (device_total - high.astype(jnp.float32)).astype(jnp.bfloat16)
    wide = (device_total.shape[0], 8, VALUE_DIM)
    message = jnp.concatenate(
        [
            end_state.astype(jnp.bfloat16),
            jnp.broadcast_to(high[:, None, None], wide),
            jnp.broadcast_to(low[:, None, None], wide),
        ],
        axis=1,
    )
    total, decay = None, None
    for k in range(1, n):
        got = later(message, "sp", k).astype(jnp.float32)
        state = got[:, :KEY_DIM]
        log = got[:, KEY_DIM, :1] + got[:, KEY_DIM + 8, :1]
        if k == 1:
            total, decay = state, log
        else:
            total = total + jnp.exp(decay)[:, :, None] * state
            decay = decay + log
    return total


def retention_finish(local_parts, state_in):
    intra_out, decayed_queries, before_local, block_ends, _, _ = local_parts
    starts = jnp.cumsum(block_ends, axis=0) - block_ends
    full_states = before_local + jnp.exp(starts)[:, :, None, None] * state_in[None]
    cross = jnp.einsum(
        "nhid,nhde->nhie",
        decayed_queries,
        full_states.astype(jnp.bfloat16),
        preferred_element_type=jnp.float32,
    )
    output = intra_out + cross
    output = output * lax.rsqrt(jnp.mean(output * output, axis=-1, keepdims=True) + EPSILON)
    blocks, heads = output.shape[:2]
    return jnp.transpose(output, (0, 2, 1, 3)).reshape(blocks * BLOCK_LEN, heads * VALUE_DIM)


def convolved(gate_c, conv_input, conv_kernel):
    tok_rows = gate_c.shape[0]
    product = gate_c.astype(jnp.float32) * conv_input.astype(jnp.float32)
    rim_rows = later(product[tok_rows - (CONV_TAPS - 1) :], "sp", 1)
    padded = jnp.concatenate([rim_rows, product], axis=0)
    out = jnp.zeros_like(product)
    for tap_index in range(CONV_TAPS):
        out = out + conv_kernel[tap_index] * padded[tap_index : tap_index + tok_rows]
    return out


def shards(
    tokens,
    norm_gain,
    query_weight,
    key_weight,
    value_weight,
    gate_weight,
    conv_b_weight,
    conv_c_weight,
    conv_in_weight,
    conv_kernel,
    out_ret_weight,
    out_conv_weight,
    log_decay,
):
    sp, fs, tp = (lax.axis_index(axis) for axis in ("sp", "fs", "tp"))

    def place(half):
        return jnp.stack([half, sp, fs, jnp.int32(lax.axis_size("fs"))]).astype(jnp.int32)

    first, second, third, fourth = pack(
        (query_weight, key_weight, value_weight),
        (conv_c_weight, conv_in_weight),
        (gate_weight, conv_b_weight),
        (out_ret_weight, out_conv_weight),
    )
    qkv_pieces = gather_line_first(first)
    ci_pieces = gather_line_first(second)
    gb_pieces = gather_line_first(third)
    out_pieces = gather_plane_first(fourth)

    normed = normalise(tokens[0], norm_gain, relative_blocks())
    qkv = project(normed, qkv_pieces)
    y, dq, message = retention(qkv, log_decay[0], place(tp))
    earlier = [later(message, "sp", k) for k in range(1, lax.axis_size("sp"))]
    conv, rim = conv_local(normed, ci_pieces, conv_kernel)
    before = later(rim[rim.shape[0] - (CONV_TAPS - 1) :], "sp", 1)
    mine, theirs = gated(normed, gb_pieces, y, dq, earlier, conv, before, conv_kernel, place(tp))
    parts = []
    for pieces in (out_pieces[:-1], out_pieces[-1:]):
        other = output_part(theirs, pieces)
        received = exchange(other, "tp", 1)
        parts += [output_part(mine, pieces), received]
    mixed = merged(parts, place(tp))
    return mixed[None]


def shards_plain(
    tokens,
    norm_gain,
    query_weight,
    key_weight,
    value_weight,
    gate_weight,
    conv_b_weight,
    conv_c_weight,
    conv_in_weight,
    conv_kernel,
    out_ret_weight,
    out_conv_weight,
    log_decay,
):
    tok_rows = tokens.shape[1]
    key_cols, value_cols = query_weight.shape[1], value_weight.shape[1]
    x = tokens[0].astype(jnp.float32)
    normed = x * lax.rsqrt(jnp.mean(x * x, axis=-1, keepdims=True) + EPSILON) * norm_gain
    normed = normed.astype(jnp.bfloat16)
    token_ordinal = (
        lax.axis_index("sp") * tok_rows + jnp.arange(tok_rows, dtype=jnp.int32)
    ).astype(jnp.float32)

    def whole(*weights):
        return lax.all_gather(
            jnp.concatenate(weights, axis=1), ("sp", "fs"), axis=0, tiled=True
        )

    def apply(*weights):
        full = jnp.dot(normed, whole(*weights), preferred_element_type=jnp.float32)
        return full.astype(jnp.bfloat16)

    qkv = apply(query_weight, key_weight, value_weight)
    local_parts = retention_local(
        (qkv[:, :key_cols], qkv[:, key_cols : 2 * key_cols], qkv[:, 2 * key_cols :]),
        log_decay[0],
        token_ordinal,
    )
    state_in = state_before(local_parts[4], local_parts[5])
    ci = apply(conv_c_weight, conv_in_weight)
    conv = convolved(ci[:, : ci.shape[1] // 2], ci[:, ci.shape[1] // 2 :], conv_kernel)
    retained = retention_finish(local_parts, state_in)
    gb = apply(gate_weight, conv_b_weight)
    ret_out = (retained * jax.nn.silu(gb[:, :value_cols].astype(jnp.float32))).astype(jnp.bfloat16)
    conv_out = (gb[:, value_cols:].astype(jnp.float32) * conv).astype(jnp.bfloat16)
    partial = lax.dot_general(
        jnp.concatenate([ret_out, conv_out], axis=1),
        whole(out_ret_weight, out_conv_weight),
        (((1,), (1,)), ((), ())),
        preferred_element_type=jnp.float32,
    )
    mixed = lax.psum_scatter(
        partial.astype(jnp.bfloat16), "tp", scatter_dimension=0, tiled=True
    )
    return mixed[None]


def takes_permutes(mesh):
    return mesh.shape["fs"] == 4 and mesh.shape["tp"] == 2 and mesh.shape["sp"] == 4


def solution(mesh):
    rows = P(("sp", "fs"), "tp")
    in_specs = (P("fs", "sp", None), P()) + (rows,) * 7 + (P(None, "tp"), rows, rows, P("fs", "tp", "sp"))
    out_specs = P("fs", ("sp", "tp"), None)
    quick = takes_permutes(mesh)
    return jax.shard_map(
        shards if quick else shards_plain,
        mesh=mesh,
        in_specs=in_specs,
        out_specs=out_specs,
        check_vma=False,
    )
```
